32 devices in a mesh: sp: 4 (over z), tp: 4 (over y, x), dp: 2 (over core).
Axes of the slice: x: 2, y: 2, z: 4, core: 2. Of those that a mesh axis runs over, the one named last changes fastest.
Arguments:
- latent: bfloat16 [8192, 2048], P(('dp', 'sp', 'tp')), parts along dimension 0, may hold values from -6 to 6
- cond: bfloat16 [4096], P('dp'), parts along dimension 0, may hold values from -6 to 6
- ctx_rows: bfloat16 [2048, 2048], P(('dp', 'sp')), parts along dimension 0, may hold values from -6 to 6
- ctx_cond: bfloat16 [2048], replicated, may hold values from -6 to 6
- mod_weight: bfloat16 [3, 2048, 2048], P(None, 'sp', 'tp'), may hold values from -0.125 to 0.125
- norm_gain: float32 [2048], replicated, may hold values from 0.1 to 1.9
- out_gain: float32 [2048], replicated, may hold values from 0.1 to 1.9
- w_query: bfloat16 [2048, 1024], replicated, may hold values from -16 to 16
- w_key: bfloat16 [2048, 256], replicated, may hold values from -1 to 1
- w_value: bfloat16 [2048, 256], replicated, may hold values from -0.125 to 0.125
- w_out: bfloat16 [1024, 2048], replicated, may hold values from -0.1875 to 0.1875
- sink: float32 [16], replicated, may hold values from 3 to 8
Outputs:
- updated: bfloat16 [8192, 2048], P(('dp', 'sp', 'tp')), parts along dimension 0
The draws below stay inside these ranges and needn't reach their ends.
There are 2 independent parts, one for each index of `dp`. The reference program is written for one: setup_inputs(seed, part) draws one part's arguments, and reference() takes and returns one part's arrays. A program takes and returns all parts, laid end to end along the dimension named above; an argument that names none is the same for every part. Nothing has to cross between parts.
All inputs are finite; a program needn't handle non-finite values.
Results may differ from the reference program's by a relative error of at most 0.0053.
Values may be sent and summed in bfloat16 or wider, within the bound.
A program may use at most 128 MiB of HBM per device.

```python
import jax
import jax.numpy as jnp
from jax import lax

D = 2048
HEADS = 16
KV_HEADS = 4
HEAD_DIM = 64
WINDOW = 128
SPAN = 128
GRID_W = 64
CTX = 1024
SEQ = 4096


def shared_weights(key):
    base_key = jax.random.fold_in(key, 11)
    first_key, second_key = jax.random.split(base_key, 2)
    key_matrix = jax.random.normal(first_key, (D, KV_HEADS * HEAD_DIM), jnp.float32) * D ** (-0.5)
    key_matrix = jnp.clip(key_matrix, -1.0, 1.0)
    query_matrix = jax.random.normal(second_key, (D, HEADS * HEAD_DIM), jnp.float32) * D ** (-0.5)
    return (key_matrix, query_matrix)


def draw_w_key(key, part):
    return shared_weights(key)[0].astype(jnp.bfloat16)


def draw_w_query(key, part):
    key_matrix, query_matrix = shared_weights(key)
    query_matrix = jnp.clip(query_matrix, -16.0, 16.0)
    return query_matrix.astype(jnp.bfloat16)


def levels(own_key, dims, cuts, least, high):
    def one(axis_at, blocks):
        steps = jax.random.uniform(jax.random.fold_in(jax.random.fold_in(own_key, 6), axis_at), (blocks,), jnp.float32, least / len(cuts), high / len(cuts))
        return jnp.repeat(jnp.exp(steps), dims[axis_at] // blocks).reshape((-1,) + (1,) * (len(dims) - axis_at - 1))

    factor_of = one(*cuts[0])
    for cut in cuts[1:]:
        factor_of = factor_of * one(*cut)
    return factor_of


def gaussian(own_key, dims, scale, most, shards=(), kind=jnp.bfloat16):
    level = levels(own_key, dims, shards, -0.22, 0.18) if shards else 1.0
    result = jax.random.normal(own_key, dims, jnp.float32) * scale * level
    return jnp.minimum(jnp.maximum(result, -most), most).astype(kind)


def setup_inputs(seed: int = 0, part: int = 0) -> dict:
    arg_keys = jax.random.split(jax.random.key(seed), 13)
    part_splits = jax.random.split(jax.random.fold_in(arg_keys[12], part), 13)
    return {
        "latent": gaussian(part_splits[0], (SEQ, D), 1.0, 6.0, ((0, 16),)),
        "cond": gaussian(part_splits[1], (D,), 1.0, 6.0),
        "ctx_rows": gaussian(part_splits[2], (CTX, D), 1.0, 6.0, ((0, 4),)),
        "ctx_cond": gaussian(arg_keys[3], (D,), 1.0, 6.0),
        "mod_weight": gaussian(arg_keys[4], (3, D, D), D ** -0.5, 0.125, ((1, 4), (2, 4))),
        "norm_gain": jnp.clip(1.0 + 0.18 * jax.random.normal(arg_keys[5], (D,), jnp.float32), 0.1, 1.9),
        "out_gain": jnp.clip(1.0 + 0.18 * jax.random.normal(arg_keys[6], (D,), jnp.float32), 0.1, 1.9),
        "w_query": draw_w_query(jax.random.fold_in(arg_keys[12], 71), part),
        "w_key": draw_w_key(jax.random.fold_in(arg_keys[12], 71), part),
        "w_value": gaussian(arg_keys[9], (D, KV_HEADS * HEAD_DIM), D ** -0.5, 0.125),
        "w_out": gaussian(arg_keys[10], (HEADS * HEAD_DIM, D), (HEADS * HEAD_DIM) ** -0.5, 0.1875),
        "sink": jnp.clip(jax.random.uniform(arg_keys[11], (HEADS,), jnp.float32, 3.0, 8.0), 3.0, 8.0),
    }


EPSILON = 1e-06
NEG_BIG = -1e+30

def rope_angles(positions, head_width):
    freq_count = head_width // 4
    inverse = 10000.0 ** (-jnp.arange(freq_count, dtype=jnp.float32) / freq_count)
    grid_row = (positions // GRID_W).astype(jnp.float32)
    grid_col = (positions % GRID_W).astype(jnp.float32)
    angles = jnp.concatenate([grid_row[:, None] * inverse, grid_col[:, None] * inverse], axis=-1)
    return (jnp.cos(angles), jnp.sin(angles))

def rotate(values, cosine, sine_table):
    half_width = values.shape[-1] // 2
    floats = values.astype(jnp.float32)
    first = floats[..., :half_width]
    second = floats[..., half_width:]
    cos_b = cosine[:, None]
    sin_b = sine_table[:, None]
    return jnp.concatenate([first * cos_b - second * sin_b, first * sin_b + second * cos_b], axis=-1).astype(jnp.bfloat16)

def mod_norm(rows, gain, scale_vec, shift_vec):
    floats = rows.astype(jnp.float32)
    normed = floats * lax.rsqrt(lax.optimization_barrier(jnp.mean(floats * floats, axis=-1, keepdims=True)) + EPSILON) * gain
    return (normed * (1.0 + scale_vec) + shift_vec).astype(jnp.bfloat16)

def band_attention(query_rot, query_plain, key_padded, value_padded, key_ctx, value_ctx, sink_group, offset, seq_total):
    length_dev, groups, head_width = query_rot.shape
    blocks = length_dev // SPAN
    query_blocks = query_rot.reshape(blocks, SPAN, groups, head_width).astype(jnp.float32)
    plain_blocks = query_plain.reshape(blocks, SPAN, groups, head_width).astype(jnp.float32)
    key_split = key_padded.reshape(blocks + 2, SPAN, head_width)
    value_split = value_padded.reshape(blocks + 2, SPAN, head_width)
    key_band = jnp.concatenate([key_split[:-2], key_split[1:-1], key_split[2:]], axis=1).astype(jnp.float32)
    value_band = jnp.concatenate([value_split[:-2], value_split[1:-1], value_split[2:]], axis=1).astype(jnp.float32)
    factor = head_width ** (-0.5)
    local = jnp.einsum('nigd,njd->ngij', query_blocks, key_band) * factor
    block_start = offset + jnp.arange(blocks, dtype=jnp.int32) * SPAN
    query_pos = block_start[:, None, None] + jnp.arange(SPAN, dtype=jnp.int32)[None, :, None]
    key_pos = block_start[:, None, None] + jnp.arange(3 * SPAN, dtype=jnp.int32)[None, None, :] - SPAN
    allowed = (jnp.abs(query_pos - key_pos) <= WINDOW) & (key_pos >= 0) & (key_pos < seq_total)
    local = jnp.where(allowed[:, None], local, NEG_BIG)
    context = jnp.einsum('nigd,cd->ngic', plain_blocks, key_ctx.astype(jnp.float32)) * factor
    sink_col = sink_group.astype(jnp.float32)[None, :, None]
    row_max = jnp.maximum(jnp.maximum(lax.optimization_barrier(jnp.max(local, axis=-1)), lax.optimization_barrier(jnp.max(context, axis=-1))), sink_col)
    exp_local = jnp.exp(local - row_max[..., None])
    exp_ctx = jnp.exp(context - row_max[..., None])
    exp_sink = jnp.exp(sink_col - row_max)
    denom = lax.optimization_barrier(jnp.sum(exp_local, axis=-1)) + lax.optimization_barrier(jnp.sum(exp_ctx, axis=-1)) + exp_sink
    weight_local = (exp_local / denom[..., None]).astype(jnp.bfloat16)
    weight_ctx = (exp_ctx / denom[..., None]).astype(jnp.bfloat16)
    mixed = jnp.einsum('ngij,njd->nigd', weight_local.astype(jnp.float32), value_band) + jnp.einsum('ngic,cd->nigd', weight_ctx.astype(jnp.float32), value_ctx.astype(jnp.float32))
    return mixed.astype(jnp.bfloat16).reshape(length_dev, groups * head_width)

def reference(latent, cond, ctx_rows, ctx_cond, mod_weight, norm_gain, out_gain, w_query, w_key, w_value, w_out, sink):
    vectors = jax.nn.silu(jnp.stack([cond, ctx_cond]).astype(jnp.float32)).astype(jnp.bfloat16)
    shift_vec = jnp.dot(vectors, mod_weight[0], preferred_element_type=jnp.float32)
    scale_vec = jnp.dot(vectors, mod_weight[1], preferred_element_type=jnp.float32)
    gate_vec = jnp.dot(vectors[:1], mod_weight[2], preferred_element_type=jnp.float32)[0]
    hidden = mod_norm(latent, norm_gain, scale_vec[0], shift_vec[0])
    ctx_hidden = mod_norm(ctx_rows, norm_gain, scale_vec[1], shift_vec[1])
    query = jnp.dot(hidden, w_query, preferred_element_type=jnp.float32).astype(jnp.bfloat16)
    keys = jnp.dot(hidden, w_key, preferred_element_type=jnp.float32).astype(jnp.bfloat16)
    values = jnp.dot(hidden, w_value, preferred_element_type=jnp.float32).astype(jnp.bfloat16)
    ctx_keys = jnp.dot(ctx_hidden, w_key, preferred_element_type=jnp.float32).astype(jnp.bfloat16)
    ctx_values = jnp.dot(ctx_hidden, w_value, preferred_element_type=jnp.float32).astype(jnp.bfloat16)
    seq_total = latent.shape[0]
    groups = HEADS // KV_HEADS
    cosine, sine_table = rope_angles(jnp.arange(seq_total, dtype=jnp.int32), HEAD_DIM)
    query_heads = query.reshape(seq_total, HEADS, HEAD_DIM)
    query_rot = rotate(query_heads, cosine, sine_table).reshape(seq_total, KV_HEADS, groups, HEAD_DIM)
    query_grid = query_heads.reshape(seq_total, KV_HEADS, groups, HEAD_DIM)
    key_rot = rotate(keys.reshape(seq_total, KV_HEADS, HEAD_DIM), cosine, sine_table)
    value_grid = values.reshape(seq_total, KV_HEADS, HEAD_DIM)
    padding = jnp.zeros((SPAN, KV_HEADS, HEAD_DIM), jnp.bfloat16)
    key_pad = jnp.concatenate([padding, key_rot, padding], axis=0)
    value_pad = jnp.concatenate([padding, value_grid, padding], axis=0)

    def one_head(operands):
        return band_attention(operands[0], operands[1], operands[2], operands[3], operands[4], operands[5], operands[6], 0, seq_total)
    stacked = lax.map(one_head, (jnp.transpose(query_rot, (1, 0, 2, 3)), jnp.transpose(query_grid, (1, 0, 2, 3)), jnp.transpose(key_pad, (1, 0, 2)), jnp.transpose(value_pad, (1, 0, 2)), jnp.transpose(ctx_keys.reshape(CTX, KV_HEADS, HEAD_DIM), (1, 0, 2)), jnp.transpose(ctx_values.reshape(CTX, KV_HEADS, HEAD_DIM), (1, 0, 2)), sink.reshape(KV_HEADS, groups)))
    mixed = jnp.transpose(stacked, (1, 0, 2)).reshape(seq_total, HEADS * HEAD_DIM)
    projected = jnp.dot(mixed, w_out, preferred_element_type=jnp.float32)
    normed = projected * lax.rsqrt(lax.optimization_barrier(jnp.mean(projected * projected, axis=-1, keepdims=True)) + EPSILON) * out_gain
    return (latent.astype(jnp.float32) + gate_vec * normed).astype(jnp.bfloat16)
```

```python
import functools
import math

import jax
import jax.numpy as jnp
from jax import lax
from jax.experimental import pallas as pl
from jax.experimental.pallas import tpu as pltpu
from jax.sharding import PartitionSpec as P

HEAD_DIM = 64
WINDOW = 128
SPAN = 128
GRID_W = 64
EPSILON = 1e-06
NEG_BIG = -1e30
LANES = 128
MESH = pl.DeviceIdType.MESH
F32 = jnp.float32
BF16 = jnp.bfloat16


def dot(a, b):
    return jnp.dot(a, b, preferred_element_type=F32)


def dot_t(a, b):
    return lax.dot_general(a, b, (((1,), (1,)), ((), ())), preferred_element_type=F32)


def kernel(
    sp_n,
    tp_n,
    latent_hbm,
    cond_ref,
    ctx_hbm,
    ctx_cond_ref,
    mod_hbm,
    norm_gain_ref,
    out_gain_ref,
    wq_hbm,
    wk_hbm,
    wv_hbm,
    wo_hbm,
    sink_ref,
    out_ref,
    mod,
    ctx,
    wkv,
    latent,
    wq,
    wo,
    hidden,
    ctx_hidden,
    silu,
    parts,
    vecs,
    rms,
    table,
    bias,
    ctx_kv,
    own_kv,
    table_t,
    own_val,
    ctx_val,
    scores,
    weights,
    q_rot,
    q_plain,
    acc,
    tops,
    mixed,
    projected,
    load_sem,
    sum_send,
    sum_recv,
    gat_send,
    gat_recv,
    z_send,
    z_recv,
    f_send,
    f_recv,
    halo_send,
    halo_recv,
):
    sp = lax.axis_index("sp")
    tp = lax.axis_index("tp")
    me = sp * tp_n + tp
    way = 1 - 2 * ((2 * sp) // sp_n)
    count = sp_n * tp_n
    rows, width = latent.shape
    ctx_rows = ctx.shape[0]
    kv_width = wkv.shape[1]
    key_width = kv_width // 2
    piece = mod.shape[1]
    cols = mod.shape[2]
    quarter = ctx_rows // tp_n
    blocks = rows // SPAN
    pairs = key_width // LANES
    heads = wq.shape[1] // HEAD_DIM
    group = heads // (key_width // HEAD_DIM)

    barrier = pltpu.get_barrier_semaphore()
    for step in range(1, count):
        other = lax.rem(me + step, count)
        pl.semaphore_signal(
            barrier,
            inc=1,
            device_id={"sp": other // tp_n, "tp": lax.rem(other, tp_n)},
            device_id_type=MESH,
        )

    loads = []
    for at, (source, target) in enumerate(
        ((mod_hbm, mod), (ctx_hbm, ctx), (wk_hbm, wkv.at[:, :key_width]), (wv_hbm, wkv.at[:, key_width:]), (latent_hbm, latent), (wq_hbm, wq), (wo_hbm, wo))
    ):
        load = pltpu.make_async_copy(source, target, load_sem.at[at])
        load.start()
        loads.append(load)

    own = []
    for which, ref in enumerate((cond_ref, ctx_cond_ref)):
        v = ref[...].astype(F32)
        silu[which] = v / (1.0 + jnp.exp(-v))
        tiles = [
            silu[which, pl.ds(sp * (piece // LANES) + i, 1)] for i in range(piece // LANES)
        ]
        own.append(jnp.broadcast_to(jnp.concatenate(tiles, axis=1), (16, piece)))
    row_id = lax.broadcasted_iota(jnp.int32, (16, piece), 0)
    loads[0].wait()
    total = None
    for which in range(3):
        left = jnp.where(
            row_id == 2 * which, own[0], jnp.where(row_id == 2 * which + 1, own[1], 0.0)
        ).astype(BF16)
        term = dot(left, mod[which])
        total = term if total is None else total + term
    parts[sp] = total[:8]
    pl.semaphore_wait(barrier, count - 1)

    def sum_copy(step, slot):
        return pltpu.make_async_remote_copy(
            src_ref=parts.at[sp],
            dst_ref=parts.at[slot],
            send_sem=sum_send.at[step - 1],
            recv_sem=sum_recv.at[slot],
            device_id={"sp": lax.rem(sp + step, sp_n), "tp": tp},
            device_id_type=MESH,
        )

    for step in range(1, sp_n):
        sum_copy(step, sp).start()

    def row_rms(ref, at):
        x = ref[...].astype(F32)
        mean = jnp.sum(x * x, axis=-1, keepdims=True) * (1.0 / width)
        rms[at, : ref.shape[0]] = jnp.broadcast_to(lax.rsqrt(mean + EPSILON), (ref.shape[0], LANES))

    loads[1].wait()
    row_rms(ctx, 1)

    for step in range(1, sp_n):
        sum_copy(step, lax.rem(sp + step, sp_n)).wait_recv()
    summed = parts[0]
    for s in range(1, sp_n):
        summed = summed + parts[s]
    vecs[tp] = summed

    def gat_copy(step, slot):
        return pltpu.make_async_remote_copy(
            src_ref=vecs.at[tp],
            dst_ref=vecs.at[slot],
            send_sem=gat_send.at[step - 1],
            recv_sem=gat_recv.at[slot],
            device_id={"sp": sp, "tp": lax.rem(tp + step, tp_n)},
            device_id_type=MESH,
        )

    for step in range(1, tp_n):
        gat_copy(step, tp).start()

    loads[4].wait()
    row_rms(latent, 0)

    lane = lax.broadcasted_iota(jnp.int32, (rows, LANES), 1)
    low_half = (lane & (HEAD_DIM // 2)) == 0
    position = me * rows + lax.broadcasted_iota(jnp.int32, (rows, LANES), 0)
    freqs = HEAD_DIM // 4
    slot = (lane & (freqs - 1)).astype(F32)
    coord = jnp.where((lane & freqs) == 0, position // GRID_W, position % GRID_W).astype(F32)
    angle = coord * jnp.exp(slot * (-math.log(10000.0) / freqs))
    table[0] = jnp.cos(angle)
    sine = jnp.sin(angle)
    table[1] = jnp.where(low_half, -sine, sine)
    half = HEAD_DIM // 2
    row_t = lax.broadcasted_iota(jnp.int32, (half, rows), 0)
    pos_t = me * rows + lax.broadcasted_iota(jnp.int32, (half, rows), 1)
    slot_t = (row_t & (freqs - 1)).astype(F32)
    coord_t = jnp.where((row_t & freqs) == 0, pos_t // GRID_W, pos_t % GRID_W).astype(F32)
    angle_t = coord_t * jnp.exp(slot_t * (-math.log(10000.0) / freqs))
    table_t[0] = jnp.cos(angle_t)
    table_t[1] = jnp.sin(angle_t)
    k_at = lax.broadcasted_iota(jnp.int32, (SPAN, SPAN), 0)
    q_at = lax.broadcasted_iota(jnp.int32, (SPAN, SPAN), 1)
    for b in range(blocks):
        for side, shift in ((0, -SPAN), (1, SPAN)):
            k_pos = me * rows + b * SPAN + k_at + shift
            ok = (jnp.abs(q_at - k_at - shift) <= WINDOW) & (k_pos >= 0) & (k_pos < count * rows)
            bias[b, side] = jnp.where(ok, 0.0, NEG_BIG)
    own_val[:, HEAD_DIM:] = jnp.ones((own_val.shape[0], own_val.shape[1] - HEAD_DIM, own_val.shape[2]), BF16)
    ctx_val[:, :, HEAD_DIM:] = jnp.ones(
        (sp_n, ctx_val.shape[1], ctx_val.shape[2] - HEAD_DIM, ctx_rows), BF16
    )
    q_rot[...] = jnp.zeros_like(q_rot)
    q_plain[...] = jnp.zeros_like(q_plain)

    for step in range(1, tp_n):
        gat_copy(step, lax.rem(tp + step, tp_n)).wait_recv()

    def modulate(ref, target, which, first, size):
        at_rows = pl.ds(first, size)
        r = rms[which, at_rows]
        r = jnp.concatenate([r] * (cols // LANES), axis=1)
        for t in range(tp_n):
            at = pl.ds(t * cols, cols)
            gain = norm_gain_ref[:, at] * (1.0 + vecs[t, 2 + which : 3 + which])
            shift = vecs[t, which : which + 1]
            target[at_rows, at] = (ref[at_rows, at].astype(F32) * r * gain + shift).astype(BF16)

    def ctx_part(t):
        first = pl.multiple_of(t * quarter, 16)
        modulate(ctx, ctx_hidden, 1, first, quarter)
        at = pl.ds(pl.multiple_of(sp * ctx_rows + t * quarter, 16), quarter)
        ctx_kv[at] = dot(ctx_hidden[pl.ds(first, quarter)], wkv[...]).astype(BF16)

    ctx_at = pl.ds(pl.multiple_of(sp * ctx_rows, 16), ctx_rows)
    loads[2].wait()
    loads[3].wait()
    ctx_part(tp)

    def peer(step):
        return lax.rem(sp + way * step + sp_n, sp_n)

    def share(s, t):
        return ctx_kv.at[pl.ds(pl.multiple_of(s * ctx_rows + t * quarter, 16), quarter)]

    def z_copy(step, s):
        return pltpu.make_async_remote_copy(
            src_ref=share(s, tp),
            dst_ref=share(s, tp),
            send_sem=z_send.at[step - 1],
            recv_sem=z_recv.at[s],
            device_id={"sp": peer(step), "tp": tp},
            device_id_type=MESH,
        )

    def f_copy(far, step, s, t):
        return pltpu.make_async_remote_copy(
            src_ref=share(s, t),
            dst_ref=share(s, t),
            send_sem=f_send.at[(far - 1) * (tp_n - 1) + step - 1],
            recv_sem=f_recv.at[s * tp_n + t],
            device_id={"sp": sp, "tp": lax.rem(tp + step, tp_n)},
            device_id_type=MESH,
        )

    for step in range(1, sp_n):
        z_copy(step, sp).start()

    def rotate(x):
        swapped = jnp.where(
            low_half, pltpu.roll(x, LANES - HEAD_DIM // 2, 1), pltpu.roll(x, HEAD_DIM // 2, 1)
        )
        return x * table[0] + swapped * table[1]

    modulate(latent, hidden, 0, 0, rows)
    kv = dot(hidden[...], wkv[...]).astype(BF16)
    for p in range(pairs):
        at = slice(p * LANES, (p + 1) * LANES)
        own_kv[SPAN : SPAN + rows, at] = rotate(kv[:, at].astype(F32)).astype(BF16)
    own_kv[SPAN : SPAN + rows, key_width:] = kv[:, key_width:]

    after = lax.rem(me + 1, count)
    before = lax.rem(me + count - 1, count)
    to_next = pltpu.make_async_remote_copy(
        src_ref=own_kv.at[pl.ds(rows, SPAN)],
        dst_ref=own_kv.at[pl.ds(0, SPAN)],
        send_sem=halo_send.at[0],
        recv_sem=halo_recv.at[0],
        device_id={"sp": after // tp_n, "tp": lax.rem(after, tp_n)},
        device_id_type=MESH,
    )
    to_prev = pltpu.make_async_remote_copy(
        src_ref=own_kv.at[pl.ds(SPAN, SPAN)],
        dst_ref=own_kv.at[pl.ds(SPAN + rows, SPAN)],
        send_sem=halo_send.at[1],
        recv_sem=halo_recv.at[1],
        device_id={"sp": before // tp_n, "tp": lax.rem(before, tp_n)},
        device_id_type=MESH,
    )

    @pl.when(me < count - 1)
    def _():
        to_next.start()

    @pl.when(me > 0)
    def _():
        to_prev.start()

    @pl.when(me == 0)
    def _():
        own_kv[:SPAN] = jnp.zeros((SPAN, kv_width), BF16)

    @pl.when(me == count - 1)
    def _():
        own_kv[SPAN + rows :] = jnp.zeros((SPAN, kv_width), BF16)

    kv_heads = heads // group
    tile = group * HEAD_DIM

    def forward(far):
        s = peer(far)
        z_copy(far, s).wait_recv()
        for step in range(1, tp_n):
            f_copy(far, step, s, tp).start()

    loads[5].wait()
    cos_t, sin_t = table_t[0], table_t[1]
    for kv in range(kv_heads):
        q = dot(hidden[...], wq[:, kv * tile : (kv + 1) * tile]) * (HEAD_DIM**-0.5)
        q_t = jnp.transpose(q.astype(BF16)).astype(F32)
        base = (kv % 2) * HEAD_DIM
        for g in range(group):
            h = kv * group + g
            x1 = q_t[g * HEAD_DIM : g * HEAD_DIM + half]
            x2 = q_t[g * HEAD_DIM + half : (g + 1) * HEAD_DIM]
            q_plain[h, base : base + half] = x1.astype(BF16)
            q_plain[h, base + half : base + HEAD_DIM] = x2.astype(BF16)
            r1 = (x1 * cos_t - x2 * sin_t).astype(BF16)
            r2 = (x1 * sin_t + x2 * cos_t).astype(BF16)
            side = slice(g * SPAN, (g + 1) * SPAN)
            for b in range(blocks):
                i = kv * blocks + b
                q_rot[i, base : base + half, side] = r1[:, b * SPAN : (b + 1) * SPAN]
                q_rot[i, base + half : base + HEAD_DIM, side] = r2[:, b * SPAN : (b + 1) * SPAN]

    for step in range(1, tp_n):
        ctx_part(lax.rem(tp + step, tp_n))
    forward(1)

    def turn(source, at, target):
        for p in range(pairs):
            v_t = jnp.transpose(source[at, key_width + p * LANES : key_width + (p + 1) * LANES])
            target[2 * p, :HEAD_DIM] = v_t[:HEAD_DIM]
            target[2 * p + 1, :HEAD_DIM] = v_t[HEAD_DIM:]

    def key_lanes(kv):
        return slice(kv // 2 * LANES, (kv // 2 + 1) * LANES)

    def state(ref, parts):
        return jnp.concatenate([ref[h, :, at] for h, at in parts], axis=1)

    def unit(parts, keys, query, bands, value, first):
        wide = sum(at.stop - at.start for _, at in parts)
        memo = {}

        def score(buf):
            k = keys()
            s = dot(k, query())
            if bands is not None:
                low, high = (jnp.concatenate([bias[bands, i]] * (wide // SPAN), axis=1) for i in range(2))
                s = jnp.concatenate([s[:SPAN] + low, s[SPAN : 2 * SPAN], s[2 * SPAN :] + high], axis=0)
            memo["size"] = s.shape[0]
            scores[buf, : s.shape[0], :wide] = s
            memo["most"] = jnp.max(s, axis=0, keepdims=True)

        def soften(buf):
            s = scores[buf, : memo["size"], :wide]
            if first:
                old = jnp.concatenate([jnp.full((1, at.stop - at.start), sink_ref[h], F32) for h, at in parts], axis=1)
            else:
                old = state(tops, parts)
            top = jnp.maximum(old, memo["most"])
            weights[buf, : memo["size"], :wide] = jnp.exp(s - top).astype(BF16)
            memo["decay"] = jnp.exp(old - top)
            col = 0
            for h, at in parts:
                size = at.stop - at.start
                tops[h, :, at] = top[:, col : col + size]
                col += size

        def mix(buf):
            term = dot(value(), weights[buf, : memo["size"], :wide])
            decay = memo["decay"]
            col = 0
            for h, at in parts:
                size = at.stop - at.start
                here = slice(col, col + size)
                if first:
                    acc[h, :HEAD_DIM, at] = term[:HEAD_DIM, here]
                    acc[h, HEAD_DIM:, at] = term[HEAD_DIM:, here] + decay[:, here]
                else:
                    acc[h, :, at] = acc[h, :, at] * decay[:, here] + term[:, here]
                col += size

        return score, soften, mix

    def context_units(at, slot, first):
        units = []
        for pair in range(heads // 2):
            kv = 2 * pair // group
            units.append(
                unit(
                    [(2 * pair, slice(0, rows)), (2 * pair + 1, slice(0, rows))],
                    lambda kv=kv: ctx_kv[at, key_lanes(kv)],
                    lambda pair=pair: jnp.concatenate([q_plain[2 * pair], q_plain[2 * pair + 1]], axis=1),
                    None,
                    lambda kv=kv: ctx_val[slot, kv],
                    first,
                )
            )
        return units

    def window_units():
        units = []
        for kv in range(kv_heads):
            for b in range(blocks):
                band = slice(b * SPAN, (b + 3) * SPAN)
                units.append(
                    unit(
                        [(kv * group + g, slice(b * SPAN, (b + 1) * SPAN)) for g in range(group)],
                        lambda kv=kv, band=band: own_kv[band, key_lanes(kv)],
                        lambda kv=kv, b=b: q_rot[kv * blocks + b],
                        b,
                        lambda kv=kv, band=band: own_val[kv, :, band],
                        False,
                    )
                )
        return units

    def run(units, before):
        for i in range(len(units) + 2):
            if i in before:
                before[i]()
            if i < len(units):
                units[i][0](i % 2)
            if 0 <= i - 1 < len(units):
                units[i - 1][1]((i - 1) % 2)
            if 0 <= i - 2 < len(units):
                units[i - 2][2](i % 2)

    def halo():
        @pl.when(me > 0)
        def _():
            to_next.wait_recv()

        @pl.when(me < count - 1)
        def _():
            to_prev.wait_recv()

        turn(own_kv, slice(None), own_val)

    def arrive(far):
        s = peer(far)
        for step in range(1, tp_n):
          f_copy(far, step, s, lax.rem(tp + step, tp_n)).wait_recv()
        at = pl.ds(pl.multiple_of(s * ctx_rows, 16), ctx_rows)
        turn(ctx_kv, at, ctx_val.at[far])
        return at

    turn(ctx_kv, ctx_at, ctx_val.at[0])
    units = context_units(ctx_at, 0, True)
    after_own = len(units)
    units += window_units()

    def second():
        if sp_n > 2:
            forward(2)
        halo()

    run(units, {after_own: second})
    for far in range(3, sp_n):
        forward(far)

    if sp_n <= 4:
        units, before = [], {}
        for far in range(1, sp_n):
            before[len(units)] = functools.partial(arrive, far)
            at = pl.ds(pl.multiple_of(peer(far) * ctx_rows, 16), ctx_rows)
            units += context_units(at, far, False)
        run(units, before)
    else:

        def far_block(far, carry):
            run(context_units(arrive(far), far, False), {})
            return carry

        lax.fori_loop(1, sp_n, far_block, 0)

    for pair in range(heads // 2):
        both = []
        for h in (2 * pair, 2 * pair + 1):
            both.append(acc[h, :HEAD_DIM] * (1.0 / acc[h, HEAD_DIM : HEAD_DIM + 1]))
        both = jnp.concatenate(both, axis=0).astype(BF16)
        mixed[:, pair * LANES : (pair + 1) * LANES] = jnp.transpose(both)

    loads[6].wait()
    wide = 256
    squares = jnp.zeros((rows, 1), F32)
    for at in range(width // wide):
        lanes = slice(at * wide, (at + 1) * wide)
        y = dot(mixed[...], wo[:, lanes])
        projected[:, lanes] = y
        squares = squares + jnp.sum(y * y, axis=-1, keepdims=True)

    r = lax.rsqrt(squares * (1.0 / width) + EPSILON)
    for t in range(tp_n):
        at = pl.ds(t * cols, cols)
        gain = vecs[t, 4:5] * out_gain_ref[:, at]
        out_ref[:, at] = (latent[:, at].astype(F32) + projected[:, at] * r * gain).astype(BF16)

    for step in range(1, sp_n):
        sum_copy(step, sp).wait_send()
        z_copy(step, sp).wait_send()
    for step in range(1, tp_n):
        gat_copy(step, tp).wait_send()
        for far in range(1, sp_n):
            s = peer(far)
            f_copy(far, step, s, tp).wait_send()

    @pl.when(me < count - 1)
    def _():
        to_next.wait_send()

    @pl.when(me > 0)
    def _():
        to_prev.wait_send()


def solution(mesh):
    sp_n, tp_n = mesh.shape["sp"], mesh.shape["tp"]

    def shards(
        latent, cond, ctx_rows, ctx_cond, mod_weight, norm_gain, out_gain, w_query, w_key, w_value, w_out, sink
    ):
        rows, width = latent.shape
        context = ctx_rows.shape[0]
        key_width = w_key.shape[1]
        heads = w_query.shape[1] // HEAD_DIM
        kv_heads = key_width // HEAD_DIM
        cols = mod_weight.shape[2]
        any_spec = pl.BlockSpec(memory_space=pl.ANY)
        vmem = pl.BlockSpec(memory_space=pltpu.VMEM)
        dma = pltpu.SemaphoreType.DMA
        return pl.pallas_call(
            functools.partial(kernel, sp_n, tp_n),
            out_shape=jax.ShapeDtypeStruct((rows, width), BF16),
            in_specs=[
                any_spec,
                vmem,
                any_spec,
                vmem,
                any_spec,
                vmem,
                vmem,
                any_spec,
                any_spec,
                any_spec,
                any_spec,
                pl.BlockSpec(memory_space=pltpu.SMEM),
            ],
            out_specs=vmem,
            scratch_shapes=[
                pltpu.VMEM(mod_weight.shape, BF16),
                pltpu.VMEM(ctx_rows.shape, BF16),
                pltpu.VMEM((width, 2 * key_width), BF16),
                pltpu.VMEM(latent.shape, BF16),
                pltpu.VMEM(w_query.shape, BF16),
                pltpu.VMEM(w_out.shape, BF16),
                pltpu.VMEM((rows, width), BF16),
                pltpu.VMEM((context, width), BF16),
                pltpu.VMEM((2, width // LANES, LANES), F32),
                pltpu.VMEM((sp_n, 8, cols), F32),
                pltpu.VMEM((tp_n, 8, cols), F32),
                pltpu.VMEM((2, max(rows, context), LANES), F32),
                pltpu.VMEM((2, rows, LANES), F32),
                pltpu.VMEM((rows // SPAN, 2, SPAN, SPAN), F32),
                pltpu.VMEM((sp_n * context, 2 * key_width), BF16),
                pltpu.VMEM((rows + 2 * SPAN, 2 * key_width), BF16),
                pltpu.VMEM((2, HEAD_DIM // 2, rows), F32),
                pltpu.VMEM((kv_heads, HEAD_DIM + 16, rows + 2 * SPAN), BF16),
                pltpu.VMEM((sp_n, kv_heads, HEAD_DIM + 16, context), BF16),
                pltpu.VMEM((2, max(3 * SPAN, context), max(2 * rows, heads // kv_heads * SPAN)), F32),
                pltpu.VMEM((2, max(3 * SPAN, context), max(2 * rows, heads // kv_heads * SPAN)), BF16),
                pltpu.VMEM((kv_heads * (rows // SPAN), LANES, heads // kv_heads * SPAN), BF16),
                pltpu.VMEM((heads, LANES, rows), BF16),
                pltpu.VMEM((heads, HEAD_DIM + 16, rows), F32),
                pltpu.VMEM((heads, 1, rows), F32),
                pltpu.VMEM((rows, heads * HEAD_DIM), BF16),
                pltpu.VMEM((rows, width), F32),
                dma((7,)),
                dma((sp_n - 1,)),
                dma((sp_n,)),
                dma((tp_n - 1,)),
                dma((tp_n,)),
                dma((sp_n - 1,)),
                dma((sp_n,)),
                dma(((sp_n - 1) * (tp_n - 1),)),
                dma((sp_n * tp_n,)),
                dma((2,)),
                dma((2,)),
            ],
            compiler_params=pltpu.CompilerParams(
                collective_id=0, has_side_effects=True, vmem_limit_bytes=50 * 1024 * 1024
            ),
        )(*[pltpu.with_memory_space_constraint(a, pltpu.HBM) for a in (
            latent,
            cond.reshape(-1, LANES),
            ctx_rows,
            ctx_cond.reshape(-1, LANES),
            mod_weight,
            norm_gain.reshape(1, -1),
            out_gain.reshape(1, -1),
            w_query,
            w_key,
            w_value,
            w_out,
            sink,
        )])

    placed = (
        P(("dp", "sp", "tp"), None),
        P("dp"),
        P(("dp", "sp"), None),
        P(),
        P(None, "sp", "tp"),
        P(),
        P(),
        P(),
        P(),
        P(),
        P(),
        P(),
    )
    return jax.shard_map(
        shards, mesh=mesh, in_specs=placed, out_specs=P(("dp", "sp", "tp"), None), check_vma=False
    )
```

```python
import functools
import math

import jax
import jax.numpy as jnp
from jax import lax
from jax.experimental import pallas as pl
from jax.experimental.pallas import tpu as pltpu
from jax.sharding import PartitionSpec as P

HEAD_DIM = 64
WINDOW = 128
SPAN = 128
GRID_W = 64
EPSILON = 1e-06
NEG_BIG = -1e30
LANES = 128
LOG2E = math.log2(math.e)
MESH = pl.DeviceIdType.MESH
F32 = jnp.float32
BF16 = jnp.bfloat16


def dot(a, b):
    return jnp.dot(a, b, preferred_element_type=F32)


def kernel(
    sp_n,
    tp_n,
    latent_hbm,
    cond_hbm,
    ctx_hbm,
    ctx_cond_hbm,
    mod_hbm,
    norm_gain_hbm,
    out_gain_hbm,
    wq_hbm,
    wk_hbm,
    wv_hbm,
    wo_hbm,
    sink_hbm,
    out_ref,
    cond_ref,
    ctx_cond_ref,
    norm_gain_ref,
    out_gain_ref,
    sink_ref,
    small_sem,
    mod,
    ctx,
    wkv,
    latent,
    wq,
    wo,
    hidden,
    ctx_hidden,
    silu,
    parts,
    vecs,
    gate_parts,
    gates,
    rms,
    table,
    bias,
    ctx_kv,
    mine,
    own_kv,
    table_t,
    own_val,
    ctx_val,
    scores,
    weights,
    q_rot,
    q_plain,
    acc,
    tops,
    mixed,
    projected,
    load_sem,
    gate_sem,
    gate_gat_sem,
    extra_sem,
    sum_send,
    sum_recv,
    gat_send,
    gat_recv,
    z_send,
    z_recv,
    f_send,
    f_recv,
    halo_send,
    halo_recv,
):
    sp = lax.axis_index("sp")
    tp = lax.axis_index("tp")
    me = sp * tp_n + tp
    way = 1 - 2 * ((2 * sp) // sp_n)
    rich = sp_n == 4 and tp_n == 4
    inner = ((sp + 1) // 2) % 2 if rich else 0 * sp
    count = sp_n * tp_n
    rows, width = latent.shape
    ctx_rows = ctx.shape[0]
    kv_width = wkv.shape[1]
    key_width = kv_width // 2
    piece = mod.shape[1]
    cols = mod.shape[2]
    quarter = ctx_rows // tp_n
    blocks = rows // SPAN
    pairs = key_width // LANES
    heads = wq.shape[1] // HEAD_DIM
    group = heads // (key_width // HEAD_DIM)

    after = lax.rem(me + 1, count)
    before = lax.rem(me + count - 1, count)

    def partner(step):
        if rich:
            return (tp + 1 - 2 * (tp % 2), tp + 2 - 4 * (tp // 2), 3 - tp)[step - 1]
        return lax.rem(tp + step, tp_n)

    barrier = pltpu.get_barrier_semaphore()

    def greet(s, t):
        pl.semaphore_signal(barrier, inc=1, device_id={"sp": s, "tp": t}, device_id_type=MESH)

    for step in range(1, sp_n):
        greet(lax.rem(sp + step, sp_n), tp)
    for step in range(1, tp_n):
        greet(sp, lax.rem(tp + step, tp_n))

    cross_next = (tp + 1) // tp_n * (1 - (sp + 1) // sp_n)
    cross_prev = (1 - (tp + tp_n - 1) // tp_n) * ((sp + sp_n - 1) // sp_n)

    @pl.when(cross_next == 1)
    def _():
        greet(after // tp_n, lax.rem(after, tp_n))

    @pl.when(cross_prev == 1)
    def _():
        greet(before // tp_n, lax.rem(before, tp_n))

    small = [
        pltpu.make_async_copy(source, target, small_sem.at[at])
        for at, (source, target) in enumerate(
            (
                (cond_hbm, cond_ref),
                (ctx_cond_hbm, ctx_cond_ref),
                (norm_gain_hbm, norm_gain_ref),
                (out_gain_hbm, out_gain_ref),
                (sink_hbm, sink_ref),
            )
        )
    ]
    for load in small[:2]:
        load.start()
    mod_loads = []
    for which in range(3):
        load = pltpu.make_async_copy(mod_hbm.at[which], mod.at[which], load_sem.at[6 + which])
        load.start()
        mod_loads.append(load)
    for load in small[2:]:
        load.start()
    loads = []
    for at, (source, target) in enumerate(
        (
            (ctx_hbm, ctx),
            (latent_hbm, latent),
            (wk_hbm, wkv.at[:, :key_width]),
            (wv_hbm, wkv.at[:, key_width:]),
            (wq_hbm, wq),
            (wo_hbm, wo),
        )
    ):
        loads.append(pltpu.make_async_copy(source, target, load_sem.at[at]))
    ctx_load, latent_load, key_load, value_load, query_load, out_load = loads

    small[0].wait()
    small[1].wait()
    own = []
    for which, ref in enumerate((cond_ref, ctx_cond_ref)):
        v = ref[...].astype(F32)
        silu[which] = v / (1.0 + jnp.exp(-v))
        tiles = [
            silu[which, pl.ds(sp * (piece // LANES) + i, 1)] for i in range(piece // LANES)
        ]
        own.append(jnp.broadcast_to(jnp.concatenate(tiles, axis=1), (16, piece)))
    row_id = lax.broadcasted_iota(jnp.int32, (16, piece), 0)
    total = None
    for which in range(3):
        left = jnp.where(
            row_id == 2 * which, own[0], jnp.where(row_id == 2 * which + 1, own[1], 0.0)
        ).astype(BF16)
        mod_loads[which].wait()
        term = dot(left, mod[which])
        if which < 2:
            total = term if total is None else total + term
        else:
            gate = term[4:5]
    fold = cols // 2
    parts[sp] = jnp.concatenate([total[:4, :fold], total[:4, fold:]], axis=0)
    gate_rows = cols // LANES
    gate_parts[sp, :gate_rows] = jnp.concatenate(
        [gate[:, i * LANES : (i + 1) * LANES] for i in range(gate_rows)], axis=0
    )
    for load in loads:
        load.start()
    pl.semaphore_wait(barrier, sp_n + tp_n - 2 + cross_next + cross_prev)

    def sum_copy(step, slot):
        return pltpu.make_async_remote_copy(
            src_ref=parts.at[sp],
            dst_ref=parts.at[slot],
            send_sem=sum_send.at[step - 1],
            recv_sem=sum_recv.at[slot],
            device_id={"sp": lax.rem(sp + step, sp_n), "tp": tp},
            device_id_type=MESH,
        )

    def gate_sum_copy(step, slot):
        return pltpu.make_async_remote_copy(
            src_ref=gate_parts.at[sp],
            dst_ref=gate_parts.at[slot],
            send_sem=gate_sem.at[step - 1],
            recv_sem=gate_sem.at[sp_n - 1 + slot],
            device_id={"sp": lax.rem(sp + step, sp_n), "tp": tp},
            device_id_type=MESH,
        )

    def gate_copy(step, slot):
        return pltpu.make_async_remote_copy(
            src_ref=gates.at[tp],
            dst_ref=gates.at[slot],
            send_sem=gate_gat_sem.at[step - 1],
            recv_sem=gate_gat_sem.at[tp_n - 1 + slot],
            device_id={"sp": sp, "tp": lax.rem(tp + step, tp_n)},
            device_id_type=MESH,
        )

    for step in range(1, sp_n):
        sum_copy(step, sp).start()
    for step in range(1, sp_n):
        gate_sum_copy(step, sp).start()

    def row_rms(ref, at):
        x = ref[...].astype(F32)
        mean = jnp.sum(x * x, axis=-1, keepdims=True) * (1.0 / width)
        rms[at, : ref.shape[0]] = jnp.broadcast_to(lax.rsqrt(mean + EPSILON), (ref.shape[0], LANES))

    ctx_load.wait()
    row_rms(ctx, 1)

    for step in range(1, sp_n):
        sum_copy(step, lax.rem(sp + step, sp_n)).wait_recv()
    summed = parts[0]
    for s in range(1, sp_n):
        summed = summed + parts[s]
    vecs[tp] = summed

    def gat_copy(step, slot):
        return pltpu.make_async_remote_copy(
            src_ref=vecs.at[tp],
            dst_ref=vecs.at[slot],
            send_sem=gat_send.at[step - 1],
            recv_sem=gat_recv.at[slot],
            device_id={"sp": sp, "tp": partner(step)},
            device_id_type=MESH,
        )

    for step in range(1, tp_n):
        gat_copy(step, tp).start()

    latent_load.wait()
    row_rms(latent, 0)

    lane = lax.broadcasted_iota(jnp.int32, (rows, LANES), 1)
    low_half = (lane & (HEAD_DIM // 2)) == 0
    position = me * rows + lax.broadcasted_iota(jnp.int32, (rows, LANES), 0)
    freqs = HEAD_DIM // 4
    slot = (lane & (freqs - 1)).astype(F32)
    coord = jnp.where((lane & freqs) == 0, position // GRID_W, position % GRID_W).astype(F32)
    angle = coord * jnp.exp(slot * (-math.log(10000.0) / freqs))
    table[0] = jnp.cos(angle)
    sine = jnp.sin(angle)
    table[1] = jnp.where(low_half, -sine, sine)
    half = HEAD_DIM // 2
    row_t = lax.broadcasted_iota(jnp.int32, (half, rows), 0)
    pos_t = me * rows + lax.broadcasted_iota(jnp.int32, (half, rows), 1)
    slot_t = (row_t & (freqs - 1)).astype(F32)
    coord_t = jnp.where((row_t & freqs) == 0, pos_t // GRID_W, pos_t % GRID_W).astype(F32)
    angle_t = coord_t * jnp.exp(slot_t * (-math.log(10000.0) / freqs))
    table_t[0] = jnp.cos(angle_t)
    table_t[1] = jnp.sin(angle_t)
    k_at = lax.broadcasted_iota(jnp.int32, (SPAN, SPAN), 0)
    q_at = lax.broadcasted_iota(jnp.int32, (SPAN, SPAN), 1)
    for b in range(blocks):
        for side, shift in ((0, -SPAN), (1, SPAN)):
            k_pos = me * rows + b * SPAN + k_at + shift
            ok = (jnp.abs(q_at - k_at - shift) <= WINDOW) & (k_pos >= 0) & (k_pos < count * rows)
            bias[b, side] = jnp.where(ok, 0.0, NEG_BIG)
    own_val[:, HEAD_DIM:] = jnp.ones((own_val.shape[0], own_val.shape[1] - HEAD_DIM, own_val.shape[2]), BF16)
    ctx_val[:, :, HEAD_DIM:] = jnp.ones(
        (sp_n, ctx_val.shape[1], ctx_val.shape[2] - HEAD_DIM, ctx_rows), BF16
    )
    q_rot[...] = jnp.zeros_like(q_rot)
    q_plain[...] = jnp.zeros_like(q_plain)

    def modulate(ref, target, which, first, size, t):
        at_rows = pl.ds(first, size)
        r = rms[which, at_rows]
        r = jnp.concatenate([r] * (fold // LANES), axis=1)
        for i in range(2):
            at = pl.ds(pl.multiple_of(t * cols + i * fold, LANES), fold)
            low = 4 * i + which
            gain = norm_gain_ref[:, at] * (1.0 + vecs[t, low + 2 : low + 3])
            shift = vecs[t, low : low + 1]
            target[at_rows, at] = (ref[at_rows, at].astype(F32) * r * gain + shift).astype(BF16)

    def ctx_rows_of(t):
        return pl.ds(pl.multiple_of(sp * ctx_rows + t * quarter, 16), quarter)

    for load in small[2:]:
        load.wait()
    key_load.wait()
    value_load.wait()
    first = pl.multiple_of(tp * quarter, 16)
    total = None
    for step in range(tp_n):
        t = tp if step == 0 else partner(step)
        if step > 0:
            gat_copy(step, t).wait_recv()
        modulate(ctx, ctx_hidden, 1, first, quarter, t)
        features = pl.ds(pl.multiple_of(t * cols, LANES), cols)
        term = dot(ctx_hidden[pl.ds(first, quarter), features], wkv[features])
        total = term if total is None else total + term
    ctx_kv[ctx_rows_of(tp)] = total.astype(BF16)

    def peer(step):
        if rich:
            step = (1, 2 + inner, 3 - inner)[step - 1]
        return lax.rem(sp + way * step + sp_n, sp_n)

    def share(s, t):
        return ctx_kv.at[pl.ds(pl.multiple_of(s * ctx_rows + t * quarter, 16), quarter)]

    def z_copy(step, s):
        return pltpu.make_async_remote_copy(
            src_ref=share(s, tp),
            dst_ref=share(s, tp),
            send_sem=z_send.at[step - 1],
            recv_sem=z_recv.at[s],
            device_id={"sp": peer(step), "tp": tp},
            device_id_type=MESH,
        )

    def f_copy(far, step, s, t, back=False):
        sent = tp_n - step if back and not rich else step
        return pltpu.make_async_remote_copy(
            src_ref=share(s, t),
            dst_ref=share(s, t),
            send_sem=f_send.at[(far - 1) * (tp_n - 1) + step - 1],
            recv_sem=f_recv.at[(far - 1) * (tp_n - 1) + sent - 1],
            device_id={"sp": sp, "tp": partner(step)},
            device_id_type=MESH,
        )

    def extra_copy(step, s):
        return pltpu.make_async_remote_copy(
            src_ref=mine.at[pl.ds(pl.multiple_of(partner(3) * quarter, 16), quarter)],
            dst_ref=share(s, partner(3)),
            send_sem=extra_sem.at[step - 1],
            recv_sem=extra_sem.at[2 + s],
            device_id={"sp": peer(step), "tp": tp},
            device_id_type=MESH,
        )

    def is_inner(run):
        pl.when(inner == 1)(run)

    def is_outer(run):
        pl.when(inner == 0)(run)

    if rich:
        z_copy(1, sp).start()

        @is_inner
        def _():
            z_copy(2, sp).start()
            z_copy(3, sp).start()
    else:
        for step in range(1, sp_n):
            z_copy(step, sp).start()

    def rotate(x, at):
        swapped = jnp.where(
            low_half[at], pltpu.roll(x, LANES - HEAD_DIM // 2, 1), pltpu.roll(x, HEAD_DIM // 2, 1)
        )
        return x * table[0, at] + swapped * table[1, at]

    to_next = pltpu.make_async_remote_copy(
        src_ref=own_kv.at[pl.ds(rows, SPAN)],
        dst_ref=own_kv.at[pl.ds(0, SPAN)],
        send_sem=halo_send.at[0],
        recv_sem=halo_recv.at[0],
        device_id={"sp": after // tp_n, "tp": lax.rem(after, tp_n)},
        device_id_type=MESH,
    )
    to_prev = pltpu.make_async_remote_copy(
        src_ref=own_kv.at[pl.ds(SPAN, SPAN)],
        dst_ref=own_kv.at[pl.ds(SPAN + rows, SPAN)],
        send_sem=halo_send.at[1],
        recv_sem=halo_recv.at[1],
        device_id={"sp": before // tp_n, "tp": lax.rem(before, tp_n)},
        device_id_type=MESH,
    )

    for b in range(blocks):
        at_rows = slice(b * SPAN, (b + 1) * SPAN)
        for t in range(tp_n):
            modulate(latent, hidden, 0, b * SPAN, SPAN, t)
        kv = dot(hidden[at_rows], wkv[...]).astype(BF16)
        to = slice((b + 1) * SPAN, (b + 2) * SPAN)
        for p in range(pairs):
            at = slice(p * LANES, (p + 1) * LANES)
            own_kv[to, at] = rotate(kv[:, at].astype(F32), at_rows).astype(BF16)
        own_kv[to, key_width:] = kv[:, key_width:]
        if b == 0:

            @pl.when(me > 0)
            def _():
                to_prev.start()

    @pl.when(me < count - 1)
    def _():
        to_next.start()

    if rich:

        @is_outer
        def _():
            z_copy(3, sp).start()
            z_copy(2, sp).start()

    @pl.when(me == 0)
    def _():
        own_kv[:SPAN] = jnp.zeros((SPAN, kv_width), BF16)

    @pl.when(me == count - 1)
    def _():
        own_kv[SPAN + rows :] = jnp.zeros((SPAN, kv_width), BF16)

    kv_heads = heads // group
    tile = group * HEAD_DIM

    def forward(far):
        s = peer(far)
        z_copy(far, s).wait_recv()
        if not rich:
            for step in range(1, tp_n):
                f_copy(far, step, s, tp).start()
            return
        if far == 2:

            @is_outer
            def _():
                f_copy(far, 3, s, tp).start()
        elif far == 3:
            f_copy(far, 3, s, tp).start()
        for step in (1, 2):
            f_copy(far, step, s, tp).start()

    for step in range(1, sp_n):
        gate_sum_copy(step, lax.rem(sp + step, sp_n)).wait_recv()
    gate_total = gate_parts[0]
    for i in range(1, sp_n):
        gate_total = gate_total + gate_parts[i]
    gates[tp] = gate_total
    for step in range(1, tp_n):
        gate_copy(step, tp).start()

    query_load.wait()
    cos_t, sin_t = table_t[0], table_t[1]
    for kv in range(kv_heads):
        q = dot(hidden[...], wq[:, kv * tile : (kv + 1) * tile]) * (HEAD_DIM**-0.5 * LOG2E)
        q_t = jnp.transpose(q.astype(BF16)).astype(F32)
        base = (kv % 2) * HEAD_DIM
        for g in range(group):
            h = kv * group + g
            x1 = q_t[g * HEAD_DIM : g * HEAD_DIM + half]
            x2 = q_t[g * HEAD_DIM + half : (g + 1) * HEAD_DIM]
            q_plain[h, base : base + half] = x1.astype(BF16)
            q_plain[h, base + half : base + HEAD_DIM] = x2.astype(BF16)
            r1 = (x1 * cos_t - x2 * sin_t).astype(BF16)
            r2 = (x1 * sin_t + x2 * cos_t).astype(BF16)
            side = slice(g * SPAN, (g + 1) * SPAN)
            for b in range(blocks):
                i = kv * blocks + b
                q_rot[i, base : base + half, side] = r1[:, b * SPAN : (b + 1) * SPAN]
                q_rot[i, base + half : base + HEAD_DIM, side] = r2[:, b * SPAN : (b + 1) * SPAN]

    for step in range(1, tp_n):
        for t in range(tp_n):
            modulate(ctx, ctx_hidden, 1, pl.multiple_of(partner(step) * quarter, 16), quarter, t)
    mine[...] = dot(ctx_hidden[...], wkv[...]).astype(BF16)
    if rich:
        extra_copy(1, sp).start()
        is_inner(lambda: extra_copy(2, sp).start())
    forward(1)
    if rich:
        is_inner(lambda: forward(2))

    def turn(source, at, target):
        for p in range(pairs):
            v_t = jnp.transpose(source[at, key_width + p * LANES : key_width + (p + 1) * LANES])
            target[2 * p, :HEAD_DIM] = v_t[:HEAD_DIM]
            target[2 * p + 1, :HEAD_DIM] = v_t[HEAD_DIM:]

    def key_lanes(kv):
        return slice(kv // 2 * LANES, (kv // 2 + 1) * LANES)

    def state(ref, parts):
        return jnp.concatenate([ref[h, :, at] for h, at in parts], axis=1)

    def unit(parts, keys, query, bands, value, first):
        wide = sum(at.stop - at.start for _, at in parts)
        memo = {}

        def score(buf):
            k = keys()
            s = dot(k, query())
            if bands is not None:
                low, high = (jnp.concatenate([bias[bands, i]] * (wide // SPAN), axis=1) for i in range(2))
                s = jnp.concatenate([s[:SPAN] + low, s[SPAN : 2 * SPAN], s[2 * SPAN :] + high], axis=0)
            memo["size"] = s.shape[0]
            scores[buf, : s.shape[0], :wide] = s
            memo["most"] = jnp.max(s, axis=0, keepdims=True)

        def soften(buf):
            s = scores[buf, : memo["size"], :wide]
            if first:
                old = jnp.concatenate([jnp.full((1, at.stop - at.start), sink_ref[h] * LOG2E, F32) for h, at in parts], axis=1)
            else:
                old = state(tops, parts)
            top = jnp.maximum(old, memo["most"])
            weights[buf, : memo["size"], :wide] = jnp.exp2(s - top).astype(BF16)
            memo["decay"] = jnp.exp2(old - top)
            col = 0
            for h, at in parts:
                size = at.stop - at.start
                tops[h, :, at] = top[:, col : col + size]
                col += size

        def mix(buf):
            term = dot(value(), weights[buf, : memo["size"], :wide])
            decay = memo["decay"]
            col = 0
            for h, at in parts:
                size = at.stop - at.start
                here = slice(col, col + size)
                if first:
                    acc[h, :HEAD_DIM, at] = term[:HEAD_DIM, here]
                    acc[h, HEAD_DIM:, at] = term[HEAD_DIM:, here] + decay[:, here]
                else:
                    acc[h, :, at] = acc[h, :, at] * decay[:, here] + term[:, here]
                col += size

        return score, soften, mix

    def context_units(source, at, slot, first):
        units = []
        for pair in range(heads // 2):
            kv = 2 * pair // group
            units.append(
                unit(
                    [(2 * pair, slice(0, rows)), (2 * pair + 1, slice(0, rows))],
                    lambda kv=kv: source[at, key_lanes(kv)],
                    lambda pair=pair: jnp.concatenate([q_plain[2 * pair], q_plain[2 * pair + 1]], axis=1),
                    None,
                    lambda kv=kv: ctx_val[slot, kv],
                    first,
                )
            )
        return units

    def window_units():
        units = []
        for kv in range(kv_heads):
            for b in range(blocks):
                band = slice(b * SPAN, (b + 3) * SPAN)
                units.append(
                    unit(
                        [(kv * group + g, slice(b * SPAN, (b + 1) * SPAN)) for g in range(group)],
                        lambda kv=kv, band=band: own_kv[band, key_lanes(kv)],
                        lambda kv=kv, b=b: q_rot[kv * blocks + b],
                        b,
                        lambda kv=kv, band=band: own_val[kv, :, band],
                        False,
                    )
                )
        return units

    def run(units, before):
        for i in range(len(units) + 2):
            if i in before:
                before[i]()
            if i < len(units):
                units[i][0](i % 2)
            if 0 <= i - 1 < len(units):
                units[i - 1][1]((i - 1) % 2)
            if 0 <= i - 2 < len(units):
                units[i - 2][2](i % 2)

    def halo():
        @pl.when(me > 0)
        def _():
            to_next.wait_recv()

        @pl.when(me < count - 1)
        def _():
            to_prev.wait_recv()

        turn(own_kv, slice(None), own_val)

    def arrive(far):
        s = peer(far)
        if rich:
            for step in (1, 2):
                f_copy(far, step, s, partner(step), True).wait_recv()
            if far == 1:
                extra_copy(far, s).wait_recv()
            elif far == 2:
                is_inner(lambda: extra_copy(far, s).wait_recv())
                is_outer(lambda: f_copy(far, 3, s, partner(3), True).wait_recv())
            else:
                f_copy(far, 3, s, partner(3), True).wait_recv()
        else:
            for step in range(1, tp_n):
                f_copy(far, step, s, partner(step), True).wait_recv()
        at = pl.ds(pl.multiple_of(s * ctx_rows, 16), ctx_rows)
        turn(ctx_kv, at, ctx_val.at[far])
        return at

    turn(mine, slice(None), ctx_val.at[0])
    units, hooks = context_units(mine, slice(None), 0, True), {}

    def remote_units(far):
        at = pl.ds(pl.multiple_of(peer(far) * ctx_rows, 16), ctx_rows)
        return context_units(ctx_kv, at, far, False)

    near = len(units)
    units += window_units()

    def relay():
        if rich:
            is_outer(lambda: forward(2))
            forward(3)
        halo()

    hooks[near] = relay
    if rich:
        for far in range(1, sp_n):

            def ready(far=far):
                arrive(far)

            hooks[len(units)] = ready
            units += remote_units(far)
        run(units, hooks)
    else:
        run(units, hooks)
        for far in range(2, sp_n):
            forward(far)

        def far_block(far, carry):
            run(context_units(ctx_kv, arrive(far), far, False), {})
            return carry

        lax.fori_loop(1, sp_n, far_block, 0)

    for pair in range(heads // 2):
        both = []
        for h in (2 * pair, 2 * pair + 1):
            both.append(acc[h, :HEAD_DIM] * (1.0 / acc[h, HEAD_DIM : HEAD_DIM + 1]))
        both = jnp.concatenate(both, axis=0).astype(BF16)
        mixed[:, pair * LANES : (pair + 1) * LANES] = jnp.transpose(both)

    out_load.wait()
    wide = 256
    squares = jnp.zeros((rows, LANES), F32)
    for at in range(width // wide):
        lanes = slice(at * wide, (at + 1) * wide)
        y = dot(mixed[...], wo[:, lanes])
        projected[:, lanes] = y
        for i in range(wide // LANES):
            part = y[:, i * LANES : (i + 1) * LANES]
            squares = squares + part * part

    for step in range(1, tp_n):
        gate_copy(step, lax.rem(tp + step, tp_n)).wait_recv()
    squares = jnp.sum(squares, axis=-1, keepdims=True)
    r = lax.rsqrt(squares * (1.0 / width) + EPSILON)
    for t in range(tp_n):
        at = pl.ds(t * cols, cols)
        gate = jnp.concatenate([gates[t, i : i + 1] for i in range(gate_rows)], axis=1)
        gain = gate * out_gain_ref[:, at]
        out_ref[:, at] = (latent[:, at].astype(F32) + projected[:, at] * r * gain).astype(BF16)

    for step in range(1, sp_n):
        sum_copy(step, sp).wait_send()
        gate_sum_copy(step, sp).wait_send()
        z_copy(step, sp).wait_send()
    for step in range(1, tp_n):
        gat_copy(step, tp).wait_send()
        gate_copy(step, tp).wait_send()
        for far in range(1, sp_n):
            done = f_copy(far, step, peer(far), tp)
            if not rich or step < 3 or far == 3:
                done.wait_send()
            elif far == 2:
                is_outer(done.wait_send)
    if rich:
        extra_copy(1, sp).wait_send()
        is_inner(lambda: extra_copy(2, sp).wait_send())

    @pl.when(me < count - 1)
    def _():
        to_next.wait_send()

    @pl.when(me > 0)
    def _():
        to_prev.wait_send()


def solution(mesh):
    sp_n, tp_n = mesh.shape["sp"], mesh.shape["tp"]

    def shards(
        latent, cond, ctx_rows, ctx_cond, mod_weight, norm_gain, out_gain, w_query, w_key, w_value, w_out, sink
    ):
        rows, width = latent.shape
        context = ctx_rows.shape[0]
        key_width = w_key.shape[1]
        heads = w_query.shape[1] // HEAD_DIM
        kv_heads = key_width // HEAD_DIM
        cols = mod_weight.shape[2]
        any_spec = pl.BlockSpec(memory_space=pl.ANY)
        vmem = pl.BlockSpec(memory_space=pltpu.VMEM)
        dma = pltpu.SemaphoreType.DMA
        return pl.pallas_call(
            functools.partial(kernel, sp_n, tp_n),
            out_shape=jax.ShapeDtypeStruct((rows, width), BF16),
            in_specs=[any_spec] * 12,
            out_specs=vmem,
            scratch_shapes=[
                pltpu.VMEM((width // LANES, LANES), BF16),
                pltpu.VMEM((width // LANES, LANES), BF16),
                pltpu.VMEM((1, width), F32),
                pltpu.VMEM((1, width), F32),
                pltpu.SMEM(sink.shape, F32),
                dma((5,)),
                pltpu.VMEM(mod_weight.shape, BF16),
                pltpu.VMEM(ctx_rows.shape, BF16),
                pltpu.VMEM((width, 2 * key_width), BF16),
                pltpu.VMEM(latent.shape, BF16),
                pltpu.VMEM(w_query.shape, BF16),
                pltpu.VMEM(w_out.shape, BF16),
                pltpu.VMEM((rows, width), BF16),
                pltpu.VMEM((context, width), BF16),
                pltpu.VMEM((2, width // LANES, LANES), F32),
                pltpu.VMEM((sp_n, 8, cols // 2), F32),
                pltpu.VMEM((tp_n, 8, cols // 2), F32),
                pltpu.VMEM((sp_n, cols // LANES, LANES), F32),
                pltpu.VMEM((tp_n, cols // LANES, LANES), F32),
                pltpu.VMEM((2, max(rows, context), LANES), F32),
                pltpu.VMEM((2, rows, LANES), F32),
                pltpu.VMEM((rows // SPAN, 2, SPAN, SPAN), F32),
                pltpu.VMEM((sp_n * context, 2 * key_width), BF16),
                pltpu.VMEM((context, 2 * key_width), BF16),
                pltpu.VMEM((rows + 2 * SPAN, 2 * key_width), BF16),
                pltpu.VMEM((2, HEAD_DIM // 2, rows), F32),
                pltpu.VMEM((kv_heads, HEAD_DIM + 16, rows + 2 * SPAN), BF16),
                pltpu.VMEM((sp_n, kv_heads, HEAD_DIM + 16, context), BF16),
                pltpu.VMEM((2, max(3 * SPAN, context), max(2 * rows, heads // kv_heads * SPAN)), F32),
                pltpu.VMEM((2, max(3 * SPAN, context), max(2 * rows, heads // kv_heads * SPAN)), BF16),
                pltpu.VMEM((kv_heads * (rows // SPAN), LANES, heads // kv_heads * SPAN), BF16),
                pltpu.VMEM((heads, LANES, rows), BF16),
                pltpu.VMEM((heads, HEAD_DIM + 16, rows), F32),
                pltpu.VMEM((heads, 1, rows), F32),
                pltpu.VMEM((rows, heads * HEAD_DIM), BF16),
                pltpu.VMEM((rows, width), F32),
                dma((9,)),
                dma((2 * sp_n - 1,)),
                dma((2 * tp_n - 1,)),
                dma((2 + sp_n,)),
                dma((sp_n - 1,)),
                dma((sp_n,)),
                dma((tp_n - 1,)),
                dma((tp_n,)),
                dma((sp_n - 1,)),
                dma((sp_n,)),
                dma(((sp_n - 1) * (tp_n - 1),)),
                dma(((sp_n - 1) * (tp_n - 1),)),
                dma((2,)),
                dma((2,)),
            ],
            compiler_params=pltpu.CompilerParams(
                collective_id=0, has_side_effects=True, vmem_limit_bytes=50 * 1024 * 1024
            ),
        )(*[pltpu.with_memory_space_constraint(a, pltpu.HBM) for a in (
            latent,
            cond.reshape(-1, LANES),
            ctx_rows,
            ctx_cond.reshape(-1, LANES),
            mod_weight,
            norm_gain.reshape(1, -1),
            out_gain.reshape(1, -1),
            w_query,
            w_key,
            w_value,
            w_out,
            sink,
        )])

    placed = (
        P(("dp", "sp", "tp"), None),
        P("dp"),
        P(("dp", "sp"), None),
        P(),
        P(None, "sp", "tp"),
        P(),
        P(),
        P(),
        P(),
        P(),
        P(),
        P(),
    )
    return jax.shard_map(
        shards, mesh=mesh, in_specs=placed, out_specs=P(("dp", "sp", "tp"), None), check_vma=False
    )
```

```python
import functools
import math

import jax
import jax.numpy as jnp
from jax import lax
from jax.experimental import pallas as pl
from jax.experimental.pallas import tpu as pltpu
from jax.sharding import PartitionSpec as P

HEAD_DIM = 64
WINDOW = 128
SPAN = 128
GRID_W = 64
EPSILON = 1e-06
NEG_BIG = -1e30
LANES = 128
LOG2E = math.log2(math.e)
MESH = pl.DeviceIdType.MESH
F32 = jnp.float32
BF16 = jnp.bfloat16


def dot(a, b):
    return jnp.dot(a, b, preferred_element_type=F32)


def kernel(
    sp_n,
    tp_n,
    latent_hbm,
    cond_hbm,
    ctx_hbm,
    ctx_cond_hbm,
    mod_hbm,
    norm_gain_hbm,
    out_gain_hbm,
    wq_hbm,
    wk_hbm,
    wv_hbm,
    wo_hbm,
    sink_hbm,
    out_ref,
    cond_ref,
    ctx_cond_ref,
    norm_gain_ref,
    out_gain_ref,
    sink_ref,
    small_sem,
    mod,
    ctx,
    wkv,
    latent,
    wq,
    wo,
    hidden,
    ctx_hidden,
    silu,
    parts,
    vecs,
    gate_parts,
    gates,
    rms,
    table,
    bias,
    ctx_kv,
    mine,
    own_kv,
    table_t,
    own_val,
    ctx_val,
    scores,
    weights,
    q_rot,
    q_plain,
    acc,
    tops,
    mixed,
    projected,
    load_sem,
    gate_sem,
    gate_gat_sem,
    extra_sem,
    sum_send,
    sum_recv,
    gat_send,
    gat_recv,
    z_send,
    z_recv,
    f_send,
    f_recv,
    halo_send,
    halo_recv,
):
    sp = lax.axis_index("sp")
    tp = lax.axis_index("tp")
    me = sp * tp_n + tp
    way = 1 - 2 * ((2 * sp) // sp_n)
    rich = sp_n == 4 and tp_n == 4
    inner = ((sp + 1) // 2) % 2 if rich else 0 * sp
    count = sp_n * tp_n
    rows, width = latent.shape
    ctx_rows = ctx.shape[0]
    kv_width = wkv.shape[1]
    key_width = kv_width // 2
    piece = mod.shape[1]
    cols = mod.shape[2]
    quarter = ctx_rows // tp_n
    blocks = rows // SPAN
    pairs = key_width // LANES
    heads = wq.shape[1] // HEAD_DIM
    group = heads // (key_width // HEAD_DIM)

    after = lax.rem(me + 1, count)
    before = lax.rem(me + count - 1, count)

    def partner(step):
        if rich:
            return (tp + 1 - 2 * (tp % 2), tp + 2 - 4 * (tp // 2), 3 - tp)[step - 1]
        return lax.rem(tp + step, tp_n)

    barrier = pltpu.get_barrier_semaphore()

    def greet(s, t):
        pl.semaphore_signal(barrier, inc=1, device_id={"sp": s, "tp": t}, device_id_type=MESH)

    for step in range(1, sp_n):
        greet(lax.rem(sp + step, sp_n), tp)
    for step in range(1, tp_n):
        greet(sp, lax.rem(tp + step, tp_n))

    cross_next = (tp + 1) // tp_n * (1 - (sp + 1) // sp_n)
    cross_prev = (1 - (tp + tp_n - 1) // tp_n) * ((sp + sp_n - 1) // sp_n)

    @pl.when(cross_next == 1)
    def _():
        greet(after // tp_n, lax.rem(after, tp_n))

    @pl.when(cross_prev == 1)
    def _():
        greet(before // tp_n, lax.rem(before, tp_n))

    small = [
        pltpu.make_async_copy(source, target, small_sem.at[at])
        for at, (source, target) in enumerate(
            (
                (cond_hbm, cond_ref),
                (ctx_cond_hbm, ctx_cond_ref),
                (norm_gain_hbm, norm_gain_ref),
                (out_gain_hbm, out_gain_ref),
                (sink_hbm, sink_ref),
            )
        )
    ]
    for load in small[:2]:
        load.start()
    mod_loads = []
    for which in range(3):
        load = pltpu.make_async_copy(mod_hbm.at[which], mod.at[which], load_sem.at[6 + which])
        load.start()
        mod_loads.append(load)
    for load in small[2:]:
        load.start()
    loads = []
    for at, (source, target) in enumerate(
        (
            (ctx_hbm, ctx),
            (latent_hbm, latent),
            (wk_hbm, wkv.at[:, :key_width]),
            (wv_hbm, wkv.at[:, key_width:]),
            (wq_hbm, wq),
            (wo_hbm, wo),
        )
    ):
        loads.append(pltpu.make_async_copy(source, target, load_sem.at[at]))
    ctx_load, latent_load, key_load, value_load, query_load, out_load = loads

    small[0].wait()
    small[1].wait()
    own = []
    for which, ref in enumerate((cond_ref, ctx_cond_ref)):
        v = ref[...].astype(F32)
        silu[which] = v / (1.0 + jnp.exp(-v))
        tiles = [
            silu[which, pl.ds(sp * (piece // LANES) + i, 1)] for i in range(piece // LANES)
        ]
        own.append(jnp.broadcast_to(jnp.concatenate(tiles, axis=1), (16, piece)))
    row_id = lax.broadcasted_iota(jnp.int32, (16, piece), 0)
    total = None
    for which in range(3):
        left = jnp.where(
            row_id == 2 * which, own[0], jnp.where(row_id == 2 * which + 1, own[1], 0.0)
        ).astype(BF16)
        mod_loads[which].wait()
        term = dot(left, mod[which])
        if which < 2:
            total = term if total is None else total + term
        else:
            gate = term[4:5]
    fold = cols // 2
    parts[sp] = jnp.concatenate([total[:4, :fold], total[:4, fold:]], axis=0)
    gate_rows = cols // LANES
    gate_parts[sp, :gate_rows] = jnp.concatenate(
        [gate[:, i * LANES : (i + 1) * LANES] for i in range(gate_rows)], axis=0
    )
    for load in loads:
        load.start()
    pl.semaphore_wait(barrier, sp_n + tp_n - 2 + cross_next + cross_prev)

    def sum_copy(step, slot):
        return pltpu.make_async_remote_copy(
            src_ref=parts.at[sp],
            dst_ref=parts.at[slot],
            send_sem=sum_send.at[step - 1],
            recv_sem=sum_recv.at[slot],
            device_id={"sp": lax.rem(sp + step, sp_n), "tp": tp},
            device_id_type=MESH,
        )

    def gate_sum_copy(step, slot):
        return pltpu.make_async_remote_copy(
            src_ref=gate_parts.at[sp],
            dst_ref=gate_parts.at[slot],
            send_sem=z_send.at[step - 1],
            recv_sem=gate_sem.at[slot],
            device_id={"sp": lax.rem(sp + step, sp_n), "tp": tp},
            device_id_type=MESH,
        )

    def gate_copy(step, slot):
        return pltpu.make_async_remote_copy(
            src_ref=gates.at[tp],
            dst_ref=gates.at[slot],
            send_sem=gat_send.at[step - 1],
            recv_sem=gate_gat_sem.at[slot],
            device_id={"sp": sp, "tp": lax.rem(tp + step, tp_n)},
            device_id_type=MESH,
        )

    for step in range(1, sp_n):
        sum_copy(step, sp).start()
    for step in range(1, sp_n):
        gate_sum_copy(step, sp).start()

    def row_rms(ref, at):
        x = ref[...].astype(F32)
        mean = jnp.sum(x * x, axis=-1, keepdims=True) * (1.0 / width)
        rms[at, : ref.shape[0]] = jnp.broadcast_to(lax.rsqrt(mean + EPSILON), (ref.shape[0], LANES))

    ctx_load.wait()
    row_rms(ctx, 1)

    for step in range(1, sp_n):
        sum_copy(step, lax.rem(sp + step, sp_n)).wait_recv()
    summed = parts[0]
    for s in range(1, sp_n):
        summed = summed + parts[s]
    vecs[tp] = summed

    def gat_copy(step, slot):
        return pltpu.make_async_remote_copy(
            src_ref=vecs.at[tp],
            dst_ref=vecs.at[slot],
            send_sem=f_send.at[step - 1],
            recv_sem=gat_recv.at[slot],
            device_id={"sp": sp, "tp": partner(step)},
            device_id_type=MESH,
        )

    for step in range(1, tp_n):
        gat_copy(step, tp).start()

    latent_load.wait()
    row_rms(latent, 0)

    lane = lax.broadcasted_iota(jnp.int32, (rows, LANES), 1)
    low_half = (lane & (HEAD_DIM // 2)) == 0
    position = me * rows + lax.broadcasted_iota(jnp.int32, (rows, LANES), 0)
    freqs = HEAD_DIM // 4
    slot = (lane & (freqs - 1)).astype(F32)
    coord = jnp.where((lane & freqs) == 0, position // GRID_W, position % GRID_W).astype(F32)
    angle = coord * jnp.exp(slot * (-math.log(10000.0) / freqs))
    table[0] = jnp.cos(angle)
    sine = jnp.sin(angle)
    table[1] = jnp.where(low_half, -sine, sine)
    half = HEAD_DIM // 2
    row_t = lax.broadcasted_iota(jnp.int32, (half, rows), 0)
    pos_t = me * rows + lax.broadcasted_iota(jnp.int32, (half, rows), 1)
    slot_t = (row_t & (freqs - 1)).astype(F32)
    coord_t = jnp.where((row_t & freqs) == 0, pos_t // GRID_W, pos_t % GRID_W).astype(F32)
    angle_t = coord_t * jnp.exp(slot_t * (-math.log(10000.0) / freqs))
    table_t[0] = jnp.cos(angle_t)
    table_t[1] = jnp.sin(angle_t)
    k_at = lax.broadcasted_iota(jnp.int32, (SPAN, SPAN), 0)
    q_at = lax.broadcasted_iota(jnp.int32, (SPAN, SPAN), 1)
    for b in range(blocks):
        for side, shift in ((0, -SPAN), (1, SPAN)):
            k_pos = me * rows + b * SPAN + k_at + shift
            ok = (jnp.abs(q_at - k_at - shift) <= WINDOW) & (k_pos >= 0) & (k_pos < count * rows)
            bias[b, side] = jnp.where(ok, 0.0, NEG_BIG)
    own_val[:, HEAD_DIM:] = jnp.ones((own_val.shape[0], own_val.shape[1] - HEAD_DIM, own_val.shape[2]), BF16)
    ctx_val[:, :, HEAD_DIM:] = jnp.ones(
        (sp_n, ctx_val.shape[1], ctx_val.shape[2] - HEAD_DIM, ctx_rows), BF16
    )
    q_rot[...] = jnp.zeros_like(q_rot)
    q_plain[...] = jnp.zeros_like(q_plain)

    def modulate(ref, target, which, first, size, t):
        at_rows = pl.ds(first, size)
        r = rms[which, at_rows]
        r = jnp.concatenate([r] * (fold // LANES), axis=1)
        for i in range(2):
            at = pl.ds(pl.multiple_of(t * cols + i * fold, LANES), fold)
            low = 4 * i + which
            gain = norm_gain_ref[:, at] * (1.0 + vecs[t, low + 2 : low + 3])
            shift = vecs[t, low : low + 1]
            target[at_rows, at] = (ref[at_rows, at].astype(F32) * r * gain + shift).astype(BF16)

    def ctx_rows_of(t):
        return pl.ds(pl.multiple_of(sp * ctx_rows + t * quarter, 16), quarter)

    for load in small[2:]:
        load.wait()
    key_load.wait()
    value_load.wait()
    first = pl.multiple_of(tp * quarter, 16)
    total = None
    for step in range(tp_n):
        t = tp if step == 0 else partner(step)
        if step > 0:
            gat_copy(step, t).wait_recv()
        modulate(ctx, ctx_hidden, 1, first, quarter, t)
        features = pl.ds(pl.multiple_of(t * cols, LANES), cols)
        term = dot(ctx_hidden[pl.ds(first, quarter), features], wkv[features])
        total = term if total is None else total + term
    ctx_kv[ctx_rows_of(tp)] = total.astype(BF16)
    for step in range(1, sp_n):
        sum_copy(step, sp).wait_send()

    def peer(step):
        if rich:
            step = (1, 2 + inner, 3 - inner)[step - 1]
        return lax.rem(sp + way * step + sp_n, sp_n)

    def share(s, t):
        return ctx_kv.at[pl.ds(pl.multiple_of(s * ctx_rows + t * quarter, 16), quarter)]

    def z_copy(step, s):
        return pltpu.make_async_remote_copy(
            src_ref=share(s, tp),
            dst_ref=share(s, tp),
            send_sem=sum_send.at[step - 1],
            recv_sem=z_recv.at[s],
            device_id={"sp": peer(step), "tp": tp},
            device_id_type=MESH,
        )

    def f_copy(far, step, s, t, back=False):
        sent = tp_n - step if back and not rich else step
        return pltpu.make_async_remote_copy(
            src_ref=share(s, t),
            dst_ref=share(s, t),
            send_sem=f_send.at[(far - 1) * (tp_n - 1) + step - 1],
            recv_sem=f_recv.at[(far - 1) * (tp_n - 1) + sent - 1],
            device_id={"sp": sp, "tp": partner(step)},
            device_id_type=MESH,
        )

    def extra_copy(step, s):
        return pltpu.make_async_remote_copy(
            src_ref=mine.at[pl.ds(pl.multiple_of(partner(3) * quarter, 16), quarter)],
            dst_ref=share(s, partner(3)),
            send_sem=extra_sem.at[step - 1],
            recv_sem=extra_sem.at[2 + s],
            device_id={"sp": peer(step), "tp": tp},
            device_id_type=MESH,
        )

    def is_inner(run):
        pl.when(inner == 1)(run)

    def is_outer(run):
        pl.when(inner == 0)(run)

    if rich:
        z_copy(1, sp).start()

        @is_inner
        def _():
            z_copy(2, sp).start()
            z_copy(3, sp).start()
    else:
        for step in range(1, sp_n):
            z_copy(step, sp).start()

    def rotate(x, at):
        swapped = jnp.where(
            low_half[at], pltpu.roll(x, LANES - HEAD_DIM // 2, 1), pltpu.roll(x, HEAD_DIM // 2, 1)
        )
        return x * table[0, at] + swapped * table[1, at]

    to_next = pltpu.make_async_remote_copy(
        src_ref=own_kv.at[pl.ds(rows, SPAN)],
        dst_ref=own_kv.at[pl.ds(0, SPAN)],
        send_sem=halo_send.at[0],
        recv_sem=halo_recv.at[0],
        device_id={"sp": after // tp_n, "tp": lax.rem(after, tp_n)},
        device_id_type=MESH,
    )
    to_prev = pltpu.make_async_remote_copy(
        src_ref=own_kv.at[pl.ds(SPAN, SPAN)],
        dst_ref=own_kv.at[pl.ds(SPAN + rows, SPAN)],
        send_sem=halo_send.at[1],
        recv_sem=halo_recv.at[1],
        device_id={"sp": before // tp_n, "tp": lax.rem(before, tp_n)},
        device_id_type=MESH,
    )

    for b in range(blocks):
        at_rows = slice(b * SPAN, (b + 1) * SPAN)
        for t in range(tp_n):
            modulate(latent, hidden, 0, b * SPAN, SPAN, t)
        kv = dot(hidden[at_rows], wkv[...]).astype(BF16)
        to = slice((b + 1) * SPAN, (b + 2) * SPAN)
        for p in range(pairs):
            at = slice(p * LANES, (p + 1) * LANES)
            own_kv[to, at] = rotate(kv[:, at].astype(F32), at_rows).astype(BF16)
        own_kv[to, key_width:] = kv[:, key_width:]
        if b == 0:

            @pl.when(me > 0)
            def _():
                to_prev.start()

    @pl.when(me < count - 1)
    def _():
        to_next.start()

    if rich:

        @is_outer
        def _():
            z_copy(3, sp).start()
            z_copy(2, sp).start()

    @pl.when(me == 0)
    def _():
        own_kv[:SPAN] = jnp.zeros((SPAN, kv_width), BF16)

    @pl.when(me == count - 1)
    def _():
        own_kv[SPAN + rows :] = jnp.zeros((SPAN, kv_width), BF16)

    kv_heads = heads // group
    tile = group * HEAD_DIM

    def forward(far):
        s = peer(far)
        z_copy(far, s).wait_recv()
        if not rich:
            for step in range(1, tp_n):
                f_copy(far, step, s, tp).start()
            return
        if far == 2:

            @is_outer
            def _():
                f_copy(far, 3, s, tp).start()
        elif far == 3:
            f_copy(far, 3, s, tp).start()
        for step in (1, 2):
            f_copy(far, step, s, tp).start()

    for step in range(1, sp_n):
        gate_sum_copy(step, lax.rem(sp + step, sp_n)).wait_recv()
    gate_total = gate_parts[0]
    for i in range(1, sp_n):
        gate_total = gate_total + gate_parts[i]
    gates[tp] = gate_total
    for step in range(1, tp_n):
        gate_copy(step, tp).start()

    query_load.wait()
    cos_t, sin_t = table_t[0], table_t[1]
    for kv in range(kv_heads):
        q = dot(hidden[...], wq[:, kv * tile : (kv + 1) * tile]) * (HEAD_DIM**-0.5 * LOG2E)
        q_t = jnp.transpose(q.astype(BF16)).astype(F32)
        base = (kv % 2) * HEAD_DIM
        for g in range(group):
            h = kv * group + g
            x1 = q_t[g * HEAD_DIM : g * HEAD_DIM + half]
            x2 = q_t[g * HEAD_DIM + half : (g + 1) * HEAD_DIM]
            q_plain[h, base : base + half] = x1.astype(BF16)
            q_plain[h, base + half : base + HEAD_DIM] = x2.astype(BF16)
            r1 = (x1 * cos_t - x2 * sin_t).astype(BF16)
            r2 = (x1 * sin_t + x2 * cos_t).astype(BF16)
            side = slice(g * SPAN, (g + 1) * SPAN)
            for b in range(blocks):
                i = kv * blocks + b
                q_rot[i, base : base + half, side] = r1[:, b * SPAN : (b + 1) * SPAN]
                q_rot[i, base + half : base + HEAD_DIM, side] = r2[:, b * SPAN : (b + 1) * SPAN]

    for step in range(1, tp_n):
        gat_copy(step, tp).wait_send()
    for step in range(1, tp_n):
        for t in range(tp_n):
            modulate(ctx, ctx_hidden, 1, pl.multiple_of(partner(step) * quarter, 16), quarter, t)
    mine[...] = dot(ctx_hidden[...], wkv[...]).astype(BF16)
    if rich:
        extra_copy(1, sp).start()
        is_inner(lambda: extra_copy(2, sp).start())
    forward(1)
    if rich:
        is_inner(lambda: forward(2))

    def turn(source, at, target):
        for p in range(pairs):
            v_t = jnp.transpose(source[at, key_width + p * LANES : key_width + (p + 1) * LANES])
            target[2 * p, :HEAD_DIM] = v_t[:HEAD_DIM]
            target[2 * p + 1, :HEAD_DIM] = v_t[HEAD_DIM:]

    def key_lanes(kv):
        return slice(kv // 2 * LANES, (kv // 2 + 1) * LANES)

    def state(ref, parts):
        return jnp.concatenate([ref[h, :, at] for h, at in parts], axis=1)

    def unit(parts, keys, query, bands, value, first):
        wide = sum(at.stop - at.start for _, at in parts)
        memo = {}

        def score(buf):
            k = keys()
            s = dot(k, query())
            if bands is not None:
                low, high = (jnp.concatenate([bias[bands, i]] * (wide // SPAN), axis=1) for i in range(2))
                s = jnp.concatenate([s[:SPAN] + low, s[SPAN : 2 * SPAN], s[2 * SPAN :] + high], axis=0)
            memo["size"] = s.shape[0]
            scores[buf, : s.shape[0], :wide] = s
            memo["most"] = jnp.max(s, axis=0, keepdims=True)

        def soften(buf):
            s = scores[buf, : memo["size"], :wide]
            if first:
                old = jnp.concatenate([jnp.full((1, at.stop - at.start), sink_ref[h] * LOG2E, F32) for h, at in parts], axis=1)
            else:
                old = state(tops, parts)
            top = jnp.maximum(old, memo["most"])
            weights[buf, : memo["size"], :wide] = jnp.exp2(s - top).astype(BF16)
            memo["decay"] = jnp.exp2(old - top)
            col = 0
            for h, at in parts:
                size = at.stop - at.start
                tops[h, :, at] = top[:, col : col + size]
                col += size

        def mix(buf):
            term = dot(value(), weights[buf, : memo["size"], :wide])
            decay = memo["decay"]
            col = 0
            for h, at in parts:
                size = at.stop - at.start
                here = slice(col, col + size)
                if first:
                    acc[h, :HEAD_DIM, at] = term[:HEAD_DIM, here]
                    acc[h, HEAD_DIM:, at] = term[HEAD_DIM:, here] + decay[:, here]
                else:
                    acc[h, :, at] = acc[h, :, at] * decay[:, here] + term[:, here]
                col += size

        return score, soften, mix

    def context_units(source, at, slot, first):
        units = []
        for pair in range(heads // 2):
            kv = 2 * pair // group
            units.append(
                unit(
                    [(2 * pair, slice(0, rows)), (2 * pair + 1, slice(0, rows))],
                    lambda kv=kv: source[at, key_lanes(kv)],
                    lambda pair=pair: jnp.concatenate([q_plain[2 * pair], q_plain[2 * pair + 1]], axis=1),
                    None,
                    lambda kv=kv: ctx_val[slot, kv],
                    first,
                )
            )
        return units

    def window_units():
        units = []
        for kv in range(kv_heads):
            for b in range(blocks):
                band = slice(b * SPAN, (b + 3) * SPAN)
                units.append(
                    unit(
                        [(kv * group + g, slice(b * SPAN, (b + 1) * SPAN)) for g in range(group)],
                        lambda kv=kv, band=band: own_kv[band, key_lanes(kv)],
                        lambda kv=kv, b=b: q_rot[kv * blocks + b],
                        b,
                        lambda kv=kv, band=band: own_val[kv, :, band],
                        False,
                    )
                )
        return units

    def run(units, before):
        for i in range(len(units) + 2):
            if i in before:
                before[i]()
            if i < len(units):
                units[i][0](i % 2)
            if 0 <= i - 1 < len(units):
                units[i - 1][1]((i - 1) % 2)
            if 0 <= i - 2 < len(units):
                units[i - 2][2](i % 2)

    def halo():
        @pl.when(me > 0)
        def _():
            to_next.wait_recv()

        @pl.when(me < count - 1)
        def _():
            to_prev.wait_recv()

        turn(own_kv, slice(None), own_val)

    def arrive(far):
        s = peer(far)
        if rich:
            for step in (1, 2):
                f_copy(far, step, s, partner(step), True).wait_recv()
            if far == 1:
                extra_copy(far, s).wait_recv()
            elif far == 2:
                is_inner(lambda: extra_copy(far, s).wait_recv())
                is_outer(lambda: f_copy(far, 3, s, partner(3), True).wait_recv())
            else:
                f_copy(far, 3, s, partner(3), True).wait_recv()
        else:
            for step in range(1, tp_n):
                f_copy(far, step, s, partner(step), True).wait_recv()
        at = pl.ds(pl.multiple_of(s * ctx_rows, 16), ctx_rows)
        turn(ctx_kv, at, ctx_val.at[far])
        return at

    turn(mine, slice(None), ctx_val.at[0])
    units, hooks = context_units(mine, slice(None), 0, True), {}

    def remote_units(far):
        at = pl.ds(pl.multiple_of(peer(far) * ctx_rows, 16), ctx_rows)
        return context_units(ctx_kv, at, far, False)

    near = len(units)
    units += window_units()

    def relay():
        if rich:
            is_outer(lambda: forward(2))
            forward(3)
        halo()

    hooks[near] = relay
    if rich:
        for far in range(1, sp_n):

            def ready(far=far):
                arrive(far)

            hooks[len(units)] = ready
            units += remote_units(far)
        run(units, hooks)
    else:
        run(units, hooks)
        for far in range(2, sp_n):
            forward(far)

        def far_block(far, carry):
            run(context_units(ctx_kv, arrive(far), far, False), {})
            return carry

        lax.fori_loop(1, sp_n, far_block, 0)

    for pair in range(heads // 2):
        both = []
        for h in (2 * pair, 2 * pair + 1):
            both.append(acc[h, :HEAD_DIM] * (1.0 / acc[h, HEAD_DIM : HEAD_DIM + 1]))
        both = jnp.concatenate(both, axis=0).astype(BF16)
        mixed[:, pair * LANES : (pair + 1) * LANES] = jnp.transpose(both)

    out_load.wait()
    wide = 256
    squares = jnp.zeros((rows, LANES), F32)
    for at in range(width // wide):
        lanes = slice(at * wide, (at + 1) * wide)
        y = dot(mixed[...], wo[:, lanes])
        projected[:, lanes] = y
        for i in range(wide // LANES):
            part = y[:, i * LANES : (i + 1) * LANES]
            squares = squares + part * part

    for step in range(1, tp_n):
        gate_copy(step, lax.rem(tp + step, tp_n)).wait_recv()
    squares = jnp.sum(squares, axis=-1, keepdims=True)
    r = lax.rsqrt(squares * (1.0 / width) + EPSILON)
    for t in range(tp_n):
        at = pl.ds(t * cols, cols)
        gate = jnp.concatenate([gates[t, i : i + 1] for i in range(gate_rows)], axis=1)
        gain = gate * out_gain_ref[:, at]
        out_ref[:, at] = (latent[:, at].astype(F32) + projected[:, at] * r * gain).astype(BF16)

    for step in range(1, sp_n):
        gate_sum_copy(step, sp).wait_send()
        z_copy(step, sp).wait_send()
    for step in range(1, tp_n):
        gate_copy(step, tp).wait_send()
        for far in range(1, sp_n):
            done = f_copy(far, step, peer(far), tp)
            if not rich or step < 3 or far == 3:
                done.wait_send()
            elif far == 2:
                is_outer(done.wait_send)
    if rich:
        extra_copy(1, sp).wait_send()
        is_inner(lambda: extra_copy(2, sp).wait_send())

    @pl.when(me < count - 1)
    def _():
        to_next.wait_send()

    @pl.when(me > 0)
    def _():
        to_prev.wait_send()


def solution(mesh):
    sp_n, tp_n = mesh.shape["sp"], mesh.shape["tp"]

    def shards(
        latent, cond, ctx_rows, ctx_cond, mod_weight, norm_gain, out_gain, w_query, w_key, w_value, w_out, sink
    ):
        rows, width = latent.shape
        context = ctx_rows.shape[0]
        key_width = w_key.shape[1]
        heads = w_query.shape[1] // HEAD_DIM
        kv_heads = key_width // HEAD_DIM
        cols = mod_weight.shape[2]
        any_spec = pl.BlockSpec(memory_space=pl.ANY)
        vmem = pl.BlockSpec(memory_space=pltpu.VMEM)
        dma = pltpu.SemaphoreType.DMA
        return pl.pallas_call(
            functools.partial(kernel, sp_n, tp_n),
            out_shape=jax.ShapeDtypeStruct((rows, width), BF16),
            in_specs=[any_spec] * 12,
            out_specs=vmem,
            scratch_shapes=[
                pltpu.VMEM((width // LANES, LANES), BF16),
                pltpu.VMEM((width // LANES, LANES), BF16),
                pltpu.VMEM((1, width), F32),
                pltpu.VMEM((1, width), F32),
                pltpu.SMEM(sink.shape, F32),
                dma((5,)),
                pltpu.VMEM(mod_weight.shape, BF16),
                pltpu.VMEM(ctx_rows.shape, BF16),
                pltpu.VMEM((width, 2 * key_width), BF16),
                pltpu.VMEM(latent.shape, BF16),
                pltpu.VMEM(w_query.shape, BF16),
                pltpu.VMEM(w_out.shape, BF16),
                pltpu.VMEM((rows, width), BF16),
                pltpu.VMEM((context, width), BF16),
                pltpu.VMEM((2, width // LANES, LANES), F32),
                pltpu.VMEM((sp_n, 8, cols // 2), F32),
                pltpu.VMEM((tp_n, 8, cols // 2), F32),
                pltpu.VMEM((sp_n, cols // LANES, LANES), F32),
                pltpu.VMEM((tp_n, cols // LANES, LANES), F32),
                pltpu.VMEM((2, max(rows, context), LANES), F32),
                pltpu.VMEM((2, rows, LANES), F32),
                pltpu.VMEM((rows // SPAN, 2, SPAN, SPAN), F32),
                pltpu.VMEM((sp_n * context, 2 * key_width), BF16),
                pltpu.VMEM((context, 2 * key_width), BF16),
                pltpu.VMEM((rows + 2 * SPAN, 2 * key_width), BF16),
                pltpu.VMEM((2, HEAD_DIM // 2, rows), F32),
                pltpu.VMEM((kv_heads, HEAD_DIM + 16, rows + 2 * SPAN), BF16),
                pltpu.VMEM((sp_n, kv_heads, HEAD_DIM + 16, context), BF16),
                pltpu.VMEM((2, max(3 * SPAN, context), max(2 * rows, heads // kv_heads * SPAN)), F32),
                pltpu.VMEM((2, max(3 * SPAN, context), max(2 * rows, heads // kv_heads * SPAN)), BF16),
                pltpu.VMEM((kv_heads * (rows // SPAN), LANES, heads // kv_heads * SPAN), BF16),
                pltpu.VMEM((heads, LANES, rows), BF16),
                pltpu.VMEM((heads, HEAD_DIM + 16, rows), F32),
                pltpu.VMEM((heads, 1, rows), F32),
                pltpu.VMEM((rows, heads * HEAD_DIM), BF16),
                pltpu.VMEM((rows, width), F32),
                dma((9,)),
                dma((sp_n,)),
                dma((tp_n,)),
                dma((2 + sp_n,)),
                dma((sp_n - 1,)),
                dma((sp_n,)),
                dma((tp_n - 1,)),
                dma((tp_n,)),
                dma((sp_n - 1,)),
                dma((sp_n,)),
                dma(((sp_n - 1) * (tp_n - 1),)),
                dma(((sp_n - 1) * (tp_n - 1),)),
                dma((2,)),
                dma((2,)),
            ],
            compiler_params=pltpu.CompilerParams(
                collective_id=0, has_side_effects=True, vmem_limit_bytes=50 * 1024 * 1024
            ),
        )(*[pltpu.with_memory_space_constraint(a, pltpu.HBM) for a in (
            latent,
            cond.reshape(-1, LANES),
            ctx_rows,
            ctx_cond.reshape(-1, LANES),
            mod_weight,
            norm_gain.reshape(1, -1),
            out_gain.reshape(1, -1),
            w_query,
            w_key,
            w_value,
            w_out,
            sink,
        )])

    placed = (
        P(("dp", "sp", "tp"), None),
        P("dp"),
        P(("dp", "sp"), None),
        P(),
        P(None, "sp", "tp"),
        P(),
        P(),
        P(),
        P(),
        P(),
        P(),
        P(),
    )
    return jax.shard_map(
        shards, mesh=mesh, in_specs=placed, out_specs=P(("dp", "sp", "tp"), None), check_vma=False
    )
```
